32 devices in a mesh: sp: 8 (over z, core), tp: 4 (over y, x).
Axes of the slice: x: 2, y: 2, z: 4, core: 2. Of those that a mesh axis runs over, the one named last changes fastest.
Arguments:
- resid: bfloat16 [4096, 2048], P(('sp', 'tp')), may hold values from -6 to 6
- branch_input: bfloat16 [1024, 4096], P('tp', 'sp'), may hold values from -6 to 6
- gate_in: bfloat16 [1024, 4096], P('tp', 'sp'), may hold values from -6 to 6
- conv_taps: bfloat16 [4, 1024], P(None, 'tp'), may hold values from -3 to 3
- rate_weight: bfloat16 [16, 64, 64], P('tp'), may hold values from -0.75 to 0.75
- input_weight: bfloat16 [16, 64, 64], P('tp'), may hold values from -0.75 to 0.75
- decay_base: float32 [1024], P('tp')
- decay_extra: float32 [4096], P('sp'), may hold values from -2 to 0
- out_weight: bfloat16 [1024, 2048], P('tp'), may hold values from -0.1875 to 0.1875
- gain_mix: float32 [2048], replicated, may hold values from 0.1 to 1.9
- gain_pre: float32 [2048], replicated, may hold values from 0.1 to 1.9
- gain_post: float32 [2048], replicated, may hold values from 0.1 to 1.9
- expert_ids: int32 [4096, 2], P(('sp', 'tp')), may hold values from 0 to 7, as said below
- route_weight: float32 [4096, 2], P(('sp', 'tp')), may hold values from 0.2 to 1
- gate_proj: bfloat16 [8, 512, 2048], P('sp', 'tp'), may hold values from -0.125 to 0.125
- up_proj: bfloat16 [8, 512, 2048], P('sp', 'tp'), may hold values from -0.125 to 0.125
- down_proj: bfloat16 [8, 512, 2048], P('sp', 'tp'), may hold values from -0.25 to 0.25
Outputs:
- layer_out: bfloat16 [4096, 2048], P(('sp', 'tp'))
The draws below stay inside these ranges and needn't reach their ends.
Inputs may be any that keep to these rules, and one draw needn't show every extreme that they name: `expert_ids`: each row names two different experts of one group: both lie in g * 2 .. g * 2 + 1 for some g. In each aligned block of 128 rows (the rows of one device) every expert is named by exactly 32 rows.
All inputs are finite; a program needn't handle non-finite values.
Results may differ from the reference program's by a relative error of at most 0.0065.
Values may be sent and summed in bfloat16 or wider, within the bound.
A program may use at most 128 MiB of HBM per device.

```python
import math
import jax
import jax.numpy as jnp
from jax import lax

D = 2048
NB = 16
BLK = 64
R = 1024
CONV = 4
HID = 512
GROUPS = 4
TOP = 2
TOK_DEV = 128
EXPERTS = 8
EXP_GROUP = 2
TOK_SP = 512
SEQUENCE_TOKENS = 4096


def draw_decay_base(key, part):
    random_subkeys = jax.random.split(key, 3)
    fast_share = 0.5
    picked = jax.random.uniform(random_subkeys[0], (R,), jnp.float32) < fast_share
    slow_rate = jnp.exp(jax.random.uniform(random_subkeys[1], (R,), jnp.float32, math.log(0.5), 0.0)) * (2.0 * math.log(2.0) / SEQUENCE_TOKENS)
    fast_rate = jnp.exp(jax.random.uniform(random_subkeys[2], (R,), jnp.float32, math.log(0.02), math.log(0.07)))
    step_rate = jnp.where(picked, fast_rate, slow_rate)
    return (-jnp.log(jnp.expm1(step_rate / 8.0))).astype(jnp.float32)


def draw_decay_extra(key, part):
    random_subkeys = jax.random.split(key, 3)
    blocks = SEQUENCE_TOKENS // TOK_SP
    factor = jnp.exp(jax.random.uniform(random_subkeys[0], (blocks,), jnp.float32, math.log(0.5), math.log(2.0)))
    baseline_value = -jnp.repeat(factor, TOK_SP, total_repeat_length=SEQUENCE_TOKENS) * (math.log(2.0) / SEQUENCE_TOKENS)
    spike_positions = jax.random.randint(random_subkeys[1], (2,), 0, SEQUENCE_TOKENS)
    spike_depth = jnp.log(jax.random.uniform(random_subkeys[2], (2,), jnp.float32, 0.6, 0.85))
    return baseline_value.at[spike_positions].add(spike_depth).astype(jnp.float32)


def draw_expert_ids(key, part):
    blocks = SEQUENCE_TOKENS // TOK_DEV
    per_group = TOK_DEV // GROUPS
    rank_list = jnp.arange(per_group, dtype=jnp.int32)
    lane_index = rank_list % EXP_GROUP
    round_index = rank_list // EXP_GROUP
    second = (lane_index + 1 + round_index % (EXP_GROUP - 1)) % EXP_GROUP
    first_lanes = jnp.tile(lane_index, GROUPS)
    second_lanes = jnp.tile(second, GROUPS)

    def member_perm(member_key):
        return jax.random.permutation(member_key, EXP_GROUP)

    def block_routes(block_key):
        random_subkeys = jax.random.split(block_key, 4)
        group_order = jax.random.permutation(random_subkeys[0], GROUPS)
        member_order = jax.vmap(member_perm)(jax.random.split(random_subkeys[1], GROUPS))
        slot_group = jnp.repeat(group_order, per_group, total_repeat_length=TOK_DEV)
        first_pick = slot_group * EXP_GROUP + member_order[slot_group, first_lanes]
        second_pick = slot_group * EXP_GROUP + member_order[slot_group, second_lanes]
        swapped = jax.random.randint(random_subkeys[2], (TOK_DEV,), 0, 2)
        paired = jnp.stack([jnp.where(swapped == 1, second_pick, first_pick), jnp.where(swapped == 1, first_pick, second_pick)], axis=1)
        row_order = jax.random.permutation(random_subkeys[3], TOK_DEV)
        return paired[row_order]
    routes = jax.vmap(block_routes)(jax.random.split(key, blocks))
    return routes.reshape(SEQUENCE_TOKENS, TOP).astype(jnp.int32)


def block_scale(own_key, dims, cuts, low, top_value):
    def one(axis_at, shards_of):
        steps = jax.random.uniform(jax.random.fold_in(jax.random.fold_in(own_key, 6), axis_at), (shards_of,), jnp.float32, low / len(cuts), top_value / len(cuts))
        return jnp.repeat(jnp.exp(steps), dims[axis_at] // shards_of).reshape((-1,) + (1,) * (len(dims) - axis_at - 1))

    level = one(*cuts[0])
    for cut in cuts[1:]:
        level = level * one(*cut)
    return level


def centred(stream_key, shape, spread, bound, cuts=(), kind=jnp.bfloat16):
    level = block_scale(stream_key, shape, cuts, -0.22, 0.18) if cuts else 1.0
    values = jax.random.normal(stream_key, shape, jnp.float32) * spread * level
    return jnp.minimum(jnp.maximum(values, -bound), bound).astype(kind)


def setup_inputs(seed: int = 0) -> dict:
    seeds = jax.random.split(jax.random.key(seed), 18)
    resid = centred(seeds[0], (SEQUENCE_TOKENS, D), 1.0, 6.0, ((0, 32),))
    branch_input = centred(seeds[1], (R, SEQUENCE_TOKENS), 1.0, 6.0, ((0, 4), (1, 8)))
    gate_in = centred(seeds[2], (R, SEQUENCE_TOKENS), 1.0, 6.0, ((0, 4), (1, 8)))
    conv_taps = centred(seeds[3], (CONV, R), CONV ** -0.5, 3.0, ((1, 4),))
    rate_weight = centred(seeds[4], (NB, BLK, BLK), BLK ** -0.5, 0.75, ((0, 4),))
    input_weight = centred(seeds[5], (NB, BLK, BLK), BLK ** -0.5, 0.75, ((0, 4),))
    decay_base = draw_decay_base(jax.random.fold_in(seeds[17], 71), 0)
    decay_extra = draw_decay_extra(jax.random.fold_in(seeds[17], 71), 0)
    out_weight = centred(seeds[8], (R, D), R ** -0.5, 0.1875, ((0, 4),))
    gain_mix = jnp.clip(1.0 + 0.18 * jax.random.normal(seeds[9], (D,), jnp.float32), 0.1, 1.9)
    gain_pre = jnp.clip(1.0 + 0.18 * jax.random.normal(seeds[10], (D,), jnp.float32), 0.1, 1.9)
    gain_post = jnp.clip(1.0 + 0.18 * jax.random.normal(seeds[11], (D,), jnp.float32), 0.1, 1.9)
    expert_ids = draw_expert_ids(jax.random.fold_in(seeds[17], 71), 0)
    route_weight = jnp.clip(0.2 + 0.8 * jax.random.uniform(seeds[13], (SEQUENCE_TOKENS, TOP), jnp.float32) ** block_scale(seeds[13], (SEQUENCE_TOKENS, TOP), ((0, 32),), -0.2, 0.2), 0.2, 1.0)
    gate_proj = centred(seeds[14], (EXPERTS, HID, D), D ** -0.5, 0.125, ((0, 8), (1, 4)))
    up_proj = centred(seeds[15], (EXPERTS, HID, D), D ** -0.5, 0.125, ((0, 8), (1, 4)))
    down_proj = centred(seeds[16], (EXPERTS, HID, D), HID ** -0.5, 0.25, ((0, 8), (1, 4)))
    return dict(resid=resid, branch_input=branch_input, gate_in=gate_in, conv_taps=conv_taps, rate_weight=rate_weight, input_weight=input_weight, decay_base=decay_base, decay_extra=decay_extra, out_weight=out_weight, gain_mix=gain_mix, gain_pre=gain_pre, gain_post=gain_post, expert_ids=expert_ids, route_weight=route_weight, gate_proj=gate_proj, up_proj=up_proj, down_proj=down_proj)


epsilon = 1e-06
gate_power = 8.0

def normalized(values, gain):
    return values * lax.rsqrt(lax.optimization_barrier(jnp.mean(values * values, axis=-1, keepdims=True)) + epsilon) * gain.astype(jnp.float32)

def combine_pair(earlier, latter):
    return (earlier[0] * latter[0], latter[0] * earlier[1] + latter[1])

def reference(resid, branch_input, gate_in, conv_taps, rate_weight, input_weight, decay_base, decay_extra, out_weight, gain_mix, gain_pre, gain_post, expert_ids, route_weight, gate_proj, up_proj, down_proj):
    blocks = SEQUENCE_TOKENS // TOK_SP
    branch_blocks = branch_input.reshape(R, blocks, TOK_SP).transpose(1, 0, 2)
    gate_blocks = gate_in.reshape(R, blocks, TOK_SP).transpose(1, 0, 2)
    extra_blocks = decay_extra.reshape(blocks, TOK_SP)
    resid_blocks = resid.reshape(blocks, TOK_SP, D)
    filter_tap_weights = conv_taps.astype(jnp.float32)
    decay_rate = -gate_power * jax.nn.softplus(-decay_base.astype(jnp.float32))
    decay_rate_matrix = rate_weight.astype(jnp.float32)
    input_matrix = input_weight.astype(jnp.float32)

    def advance(carried, pieces):
        edge_cols, entering = carried
        branch_block, gate_block, extra_block, resid_block = pieces
        padded = jnp.concatenate([edge_cols, branch_block.astype(jnp.float32)], axis=1)
        convolved = filter_tap_weights[0][:, None] * padded[:, 0:TOK_SP]
        for offset in range(1, CONV):
            convolved = convolved + filter_tap_weights[offset][:, None] * padded[:, offset:offset + TOK_SP]
        grouped = convolved.reshape(NB, BLK, TOK_SP)
        rate_gate = jax.nn.sigmoid(jnp.einsum('ncs,ncd->nds', grouped, decay_rate_matrix, precision=lax.Precision.HIGHEST).reshape(R, TOK_SP))
        input_gate = jax.nn.sigmoid(jnp.einsum('ncs,ncd->nds', grouped, input_matrix, precision=lax.Precision.HIGHEST).reshape(R, TOK_SP))
        log_keep = decay_rate[:, None] * rate_gate + extra_block[None, :]
        retain = jnp.exp(log_keep)
        driven = jnp.sqrt(-jnp.expm1(2.0 * log_keep)) * input_gate * convolved
        retained, local_state = lax.associative_scan(combine_pair, (retain, driven), axis=1)
        hidden_state = local_state + retained * entering[:, None]
        branch_out = (hidden_state * jax.nn.gelu(gate_block.astype(jnp.float32), approximate=True)).astype(jnp.bfloat16)
        mixed_rows = lax.dot_general(branch_out, out_weight, (((0,), (0,)), ((), ())), preferred_element_type=jnp.float32)
        after_mix = resid_block.astype(jnp.float32) + normalized(mixed_rows, gain_mix)
        ffn_in = normalized(after_mix, gain_pre).astype(jnp.bfloat16)
        return ((padded[:, TOK_SP:], hidden_state[:, -1]), (after_mix, ffn_in))
    start_state = (jnp.zeros((R, CONV - 1), jnp.float32), jnp.zeros((R,), jnp.float32))
    _, (after_mix, ffn_in) = lax.scan(advance, start_state, (branch_blocks, gate_blocks, extra_blocks, resid_blocks))
    after_mix = after_mix.reshape(SEQUENCE_TOKENS, D)
    ffn_in = ffn_in.reshape(SEQUENCE_TOKENS, D)
    chosen = expert_ids.reshape(-1).astype(jnp.int32)
    matches = (chosen[:, None] == jnp.arange(EXPERTS, dtype=jnp.int32)[None, :]).astype(jnp.int32)
    slot_index = lax.optimization_barrier(jnp.sum((jnp.cumsum(matches, axis=0) - 1) * matches, axis=1))
    per_expert = SEQUENCE_TOKENS * TOP // EXPERTS
    entries = jnp.zeros((EXPERTS * per_expert,), jnp.int32).at[chosen * per_expert + slot_index].set(jnp.arange(SEQUENCE_TOKENS * TOP, dtype=jnp.int32))
    entries = entries.reshape(EXPERTS, per_expert)
    weights_flat = route_weight.astype(jnp.float32).reshape(-1)

    def expert_step(totals, pieces):
        expert, entry_list = pieces
        token_index = entry_list // TOP
        picked_rows = ffn_in[token_index]
        gate_vals = jnp.dot(picked_rows, gate_proj[expert].T, preferred_element_type=jnp.float32)
        up_vals = jnp.dot(picked_rows, up_proj[expert].T, preferred_element_type=jnp.float32)
        hidden = (jax.nn.silu(gate_vals) * up_vals).astype(jnp.bfloat16)
        result = jnp.dot(hidden, down_proj[expert], preferred_element_type=jnp.float32).astype(jnp.bfloat16)
        weighted = result.astype(jnp.float32) * weights_flat[entry_list][:, None]
        return (totals.at[token_index].add(weighted), None)
    totals, _ = lax.scan(expert_step, jnp.zeros((SEQUENCE_TOKENS, D), jnp.float32), (jnp.arange(EXPERTS, dtype=jnp.int32), entries))
    return (after_mix + normalized(totals, gain_post)).astype(jnp.bfloat16)
```

```python
import jax
import jax.numpy as jnp
from jax import lax
from jax.experimental import pallas as pl
from jax.experimental.pallas import tpu as pltpu
from jax.sharding import PartitionSpec as P

epsilon = 1e-06
gate_power = 8.0


def entering_2(array, axis, combine, identity):
    count, here = (lax.axis_size(axis), lax.axis_index(axis))
    everything = jax.tree.map(lambda part: lax.all_gather(part, axis), array)
    start = jax.tree.map(
        lambda part, zero: jnp.broadcast_to(jnp.asarray(zero, part.dtype), part.shape),
        array,
        identity,
    )

    def hop(k, before):
        reached = k < here
        new = combine(before, jax.tree.map(lambda part: part[k], everything))
        return jax.tree.map(lambda a, b: jnp.where(reached, a, b), new, before)

    return lax.fori_loop(0, count, hop, start)


def passed_along(value, axis, steps):
    count = lax.axis_size(axis)
    first, last = (max(0, -steps), min(count, count - steps))
    return lax.ppermute(value, axis, [(source, source + steps) for source in range(first, last)])


def normalized(values, gain):
    return values * lax.rsqrt(jnp.mean(values * values, axis=-1, keepdims=True) + epsilon) * gain


def combine_pair(earlier, latter):
    return (earlier[0] * latter[0], latter[0] * earlier[1] + latter[1])


def carry_in(block_keep, block_state):
    identity = (jnp.ones(block_keep.shape, jnp.float32), jnp.zeros(block_state.shape, jnp.float32))
    return entering_2((block_keep, block_state), "sp", combine_pair, identity)


def shifted(values, fill, distance, lane):
    return jnp.where(lane >= distance, pltpu.roll(values, distance, 1), fill)


def one_minus_exp(y):
    small = 1.0 + y * (1.0 / 8.0)
    for k in range(7, 1, -1):
        small = 1.0 + y * (1.0 / k) * small
    return jnp.where(y > -0.5, -y * small, 1.0 - jnp.exp(y))


def split_three(values):
    high = values.astype(jnp.bfloat16)
    rest = values - high.astype(jnp.float32)
    mid = rest.astype(jnp.bfloat16)
    low = (rest - mid.astype(jnp.float32)).astype(jnp.bfloat16)
    return high, mid, low


def scan_kernel(edge_ref, input_ref, taps_ref, rate_ref, inward_ref, decay_ref, extra_ref, keep_ref, state_ref):
    taps = taps_ref[0]
    positions = input_ref.shape[1]
    here = input_ref[...].astype(jnp.float32)
    padded = jnp.concatenate([edge_ref[...].astype(jnp.float32), here], axis=1)
    pad = padded.shape[1] - positions
    count = taps.shape[1]
    convolved = taps[:, count - 1 : count] * here
    for back in range(1, count):
        moved = pltpu.roll(padded, back, 1)[:, pad:]
        convolved = convolved + taps[:, count - 1 - back : count - back] * moved
    stacked = jnp.concatenate(split_three(convolved), axis=0)

    def gate(weight):
        return jax.nn.sigmoid(
            lax.dot_general(
                jnp.concatenate([weight] * 3, axis=0),
                stacked,
                (((0,), (0,)), ((), ())),
                preferred_element_type=jnp.float32,
            )
        )

    log_keep = decay_ref[0] * gate(rate_ref[0]) + extra_ref[...]
    state = jnp.sqrt(one_minus_exp(2.0 * log_keep)) * gate(inward_ref[0]) * convolved
    keep = jnp.exp(log_keep)
    lane = lax.broadcasted_iota(jnp.int32, keep.shape, 1)
    distance = 1
    while distance < positions:
        state = keep * shifted(state, 0.0, distance, lane) + state
        keep = keep * shifted(keep, 1.0, distance, lane)
        distance *= 2
    keep_ref[...] = keep
    state_ref[...] = state


def local_scan(edge, branch_input, conv_taps, rate_weight, input_weight, decay_rate, decay_extra):
    channels, positions = branch_input.shape
    blocks, width = rate_weight.shape[:2]
    taps = conv_taps.astype(jnp.float32).T.reshape(blocks, width, conv_taps.shape[0])
    pad = 128
    edge = jnp.pad(edge, ((0, 0), (pad - edge.shape[1], 0)))
    row = lambda i: (i, 0)
    block3 = lambda i: (i, 0, 0)
    return pl.pallas_call(
        scan_kernel,
        grid=(blocks,),
        in_specs=[
            pl.BlockSpec((width, pad), row),
            pl.BlockSpec((width, positions), row),
            pl.BlockSpec((1, width, taps.shape[2]), block3),
            pl.BlockSpec((1, width, width), block3),
            pl.BlockSpec((1, width, width), block3),
            pl.BlockSpec((1, width, 1), block3),
            pl.BlockSpec((1, positions), lambda i: (0, 0)),
        ],
        out_specs=[pl.BlockSpec((width, positions), row)] * 2,
        out_shape=[jax.ShapeDtypeStruct((channels, positions), jnp.float32)] * 2,
        cost_estimate=pl.CostEstimate(flops=channels * positions * 400, bytes_accessed=channels * positions * 12, transcendentals=channels * positions * 5),
    )(
        edge,
        branch_input,
        taps,
        rate_weight,
        input_weight,
        decay_rate.reshape(blocks, width, 1),
        decay_extra.reshape(1, positions),
    )


def expert_mlp(rows, gate_rows, up_rows, down_rows):
    contract = (((1,), (1,)), ((), ()))
    gate_vals = lax.dot_general(rows, gate_rows, contract, preferred_element_type=jnp.float32)
    up_vals = lax.dot_general(rows, up_rows, contract, preferred_element_type=jnp.float32)
    hidden = (jax.nn.silu(gate_vals) * up_vals).astype(jnp.bfloat16)
    return jnp.dot(hidden, down_rows, preferred_element_type=jnp.float32).astype(jnp.bfloat16)


def paired_moe(ffn_in, expert_ids, route_weight, gate_rows, up_rows, down_rows):
    tokens, width = ffn_in.shape
    devices = lax.axis_size("sp")
    groups = devices // 2
    cap = tokens // groups
    group = expert_ids[:, 0] // 2
    member = (group[:, None] == jnp.arange(groups, dtype=jnp.int32)[None, :]).astype(jnp.int32)
    slot = group * cap + jnp.sum((jnp.cumsum(member, axis=0) - 1) * member, axis=1)
    place = (slot[None, :] == jnp.arange(tokens, dtype=jnp.int32)[:, None]).astype(jnp.bfloat16)
    even = (expert_ids[:, 0] % 2 == 0)[:, None]
    by_expert = jnp.where(even, route_weight, route_weight[:, ::-1])
    extra = jnp.concatenate(split_three(by_expert), axis=1)
    extra = jnp.pad(extra, ((0, 0), (0, 128 - extra.shape[1])))
    outgoing = jnp.dot(place, jnp.concatenate([ffn_in, extra], axis=1), preferred_element_type=jnp.float32)
    outgoing = outgoing.astype(jnp.bfloat16)
    swap = [(i, i ^ 1) for i in range(devices)]
    mine = lax.all_to_all(outgoing, "sp", split_axis=0, concat_axis=0, tiled=True)
    rows = mine[:, :width]
    other_rows = lax.ppermute(rows, "sp", swap)
    other_out = expert_mlp(other_rows, gate_rows, up_rows, down_rows)
    from_other = lax.ppermute(other_out, "sp", swap)
    own_out = expert_mlp(rows, gate_rows, up_rows, down_rows)
    scale = mine[:, width : width + 6].astype(jnp.float32)
    scale = scale[:, 0:2] + scale[:, 2:4] + scale[:, 4:6]
    first = lax.axis_index("sp") % 2 == 0
    own_scale = jnp.where(first, scale[:, 0:1], scale[:, 1:2])
    other_scale = jnp.where(first, scale[:, 1:2], scale[:, 0:1])
    summed = own_scale * own_out.astype(jnp.float32) + other_scale * from_other.astype(jnp.float32)
    returned = lax.all_to_all(summed.astype(jnp.bfloat16), "sp", split_axis=0, concat_axis=0, tiled=True)
    return lax.dot_general(place, returned, (((0,), (0,)), ((), ())), preferred_element_type=jnp.float32)


def general_moe(ffn_in, expert_ids, route_weight, gate_rows, up_rows, down_rows):
    token_count = ffn_in.shape[0]
    top_count = expert_ids.shape[1]
    experts = gate_rows.shape[0] * lax.axis_size("sp")
    capacity = top_count * token_count // experts
    chosen = expert_ids.reshape(-1)
    matches = (chosen[:, None] == jnp.arange(experts, dtype=jnp.int32)[None, :]).astype(jnp.int32)
    slot_index = jnp.sum((jnp.cumsum(matches, axis=0) - 1) * matches, axis=1)
    target = chosen * capacity + slot_index
    source = (
        jnp.zeros((experts * capacity,), jnp.int32)
        .at[target]
        .set(jnp.arange(token_count * top_count, dtype=jnp.int32) // top_count)
    )
    outgoing = ffn_in[source].reshape(experts, capacity, ffn_in.shape[1])
    arriving = lax.all_to_all(outgoing, "sp", split_axis=0, concat_axis=1, tiled=True)
    gate_vals = jnp.einsum("emd,ekd->emk", arriving, gate_rows, preferred_element_type=jnp.float32)
    up_vals = jnp.einsum("emd,ekd->emk", arriving, up_rows, preferred_element_type=jnp.float32)
    hidden = (jax.nn.silu(gate_vals) * up_vals).astype(jnp.bfloat16)
    result = jnp.einsum("emk,ekd->emd", hidden, down_rows, preferred_element_type=jnp.float32)
    returned = lax.all_to_all(
        result.astype(jnp.bfloat16), "sp", split_axis=1, concat_axis=0, tiled=True
    )
    returned = returned.reshape(experts * capacity, returned.shape[2])
    picked = returned[target].astype(jnp.float32).reshape(token_count, top_count, returned.shape[1])
    return jnp.sum(picked * route_weight[:, :, None], axis=1)


expert_groups = 4


def per_device(
    resid,
    branch_input,
    gate_in,
    conv_taps,
    rate_weight,
    input_weight,
    decay_base,
    decay_extra,
    out_weight,
    gain_mix,
    gain_pre,
    gain_post,
    expert_ids,
    route_weight,
    gate_proj,
    up_proj,
    down_proj,
):
    channels, positions = branch_input.shape
    tap_count = conv_taps.shape[0]
    edge_cols = passed_along(branch_input[:, positions - (tap_count - 1) :], "sp", 1)
    decay_rate = -gate_power * jax.nn.softplus(-decay_base)
    keep, state = local_scan(
        edge_cols, branch_input, conv_taps, rate_weight, input_weight, decay_rate, decay_extra
    )
    _, entering = carry_in(keep[:, -1], state[:, -1])
    hidden_state = state + keep * entering[:, None]
    branch_out = (hidden_state * jax.nn.gelu(gate_in.astype(jnp.float32), approximate=True)).astype(
        jnp.bfloat16
    )
    token_rows = lax.all_to_all(branch_out, "tp", split_axis=1, concat_axis=0, tiled=True)
    token_count = token_rows.shape[1]
    mixed_rows = lax.dot_general(
        token_rows,
        lax.all_gather(out_weight, "tp", axis=0, tiled=True),
        (((0,), (0,)), ((), ())),
        preferred_element_type=jnp.float32,
    )
    after_mix = resid.astype(jnp.float32) + normalized(mixed_rows, gain_mix)
    ffn_in = normalized(after_mix, gain_pre).astype(jnp.bfloat16)
    gate_rows = lax.all_gather(gate_proj, "tp", axis=1, tiled=True)
    up_rows = lax.all_gather(up_proj, "tp", axis=1, tiled=True)
    down_rows = lax.all_gather(down_proj, "tp", axis=1, tiled=True)
    experts = gate_proj.shape[0] * lax.axis_size("sp")
    if gate_proj.shape[0] == 1 and experts // expert_groups == 2:
        moe = paired_moe(ffn_in, expert_ids, route_weight, gate_rows[0], up_rows[0], down_rows[0])
    else:
        moe = general_moe(ffn_in, expert_ids, route_weight, gate_rows, up_rows, down_rows)
    return (after_mix + normalized(moe, gain_post)).astype(jnp.bfloat16)


def solution(mesh):
    in_specs = (
        P(("sp", "tp"), None),
        P("tp", "sp"),
        P("tp", "sp"),
        P(None, "tp"),
        P("tp", None, None),
        P("tp", None, None),
        P("tp"),
        P("sp"),
        P("tp", None),
        P(),
        P(),
        P(),
        P(("sp", "tp"), None),
        P(("sp", "tp"), None),
        P("sp", "tp", None),
        P("sp", "tp", None),
        P("sp", "tp", None),
    )
    out_specs = P(("sp", "tp"), None)
    return jax.shard_map(
        per_device, mesh=mesh, in_specs=in_specs, out_specs=out_specs, check_vma=False
    )
```

```python
import jax
import jax.numpy as jnp
from jax import lax
from jax.experimental import pallas as pl
from jax.experimental.pallas import tpu as pltpu
from jax.sharding import PartitionSpec as P

epsilon = 1e-06
gate_power = 8.0


def entering_2(array, axis, combine, identity):
    count, here = (lax.axis_size(axis), lax.axis_index(axis))
    everything = jax.tree.map(lambda part: lax.all_gather(part, axis), array)
    start = jax.tree.map(
        lambda part, zero: jnp.broadcast_to(jnp.asarray(zero, part.dtype), part.shape),
        array,
        identity,
    )

    def hop(k, before):
        reached = k < here
        new = combine(before, jax.tree.map(lambda part: part[k], everything))
        return jax.tree.map(lambda a, b: jnp.where(reached, a, b), new, before)

    return lax.fori_loop(0, count, hop, start)


def passed_along(value, axis, steps):
    count = lax.axis_size(axis)
    first, last = (max(0, -steps), min(count, count - steps))
    return lax.ppermute(value, axis, [(source, source + steps) for source in range(first, last)])


def normalized(values, gain):
    return values * lax.rsqrt(jnp.mean(values * values, axis=-1, keepdims=True) + epsilon) * gain


def combine_pair(earlier, latter):
    return (earlier[0] * latter[0], latter[0] * earlier[1] + latter[1])


def carry_in(block_keep, block_state):
    identity = (jnp.ones(block_keep.shape, jnp.float32), jnp.zeros(block_state.shape, jnp.float32))
    return entering_2((block_keep, block_state), "sp", combine_pair, identity)


def shifted(values, fill, distance, lane):
    return jnp.where(lane >= distance, pltpu.roll(values, distance, 1), fill)


def one_minus_exp(y):
    small = 1.0 + y * (1.0 / 8.0)
    for k in range(7, 1, -1):
        small = 1.0 + y * (1.0 / k) * small
    return jnp.where(y > -0.5, -y * small, 1.0 - jnp.exp(y))


def split_three(values):
    high = values.astype(jnp.bfloat16)
    rest = values - high.astype(jnp.float32)
    mid = rest.astype(jnp.bfloat16)
    low = (rest - mid.astype(jnp.float32)).astype(jnp.bfloat16)
    return high, mid, low


def scan_kernel(edge_ref, input_ref, taps_ref, rate_ref, inward_ref, decay_ref, extra_ref, keep_ref, state_ref):
    taps = taps_ref[0]
    positions = input_ref.shape[1]
    here = input_ref[...].astype(jnp.float32)
    padded = jnp.concatenate([edge_ref[...].astype(jnp.float32), here], axis=1)
    pad = padded.shape[1] - positions
    count = taps.shape[1]
    convolved = taps[:, count - 1 : count] * here
    for back in range(1, count):
        moved = pltpu.roll(padded, back, 1)[:, pad:]
        convolved = convolved + taps[:, count - 1 - back : count - back] * moved
    stacked = jnp.concatenate(split_three(convolved), axis=0)

    def gate(weight):
        return jax.nn.sigmoid(
            lax.dot_general(
                jnp.concatenate([weight] * 3, axis=0),
                stacked,
                (((0,), (0,)), ((), ())),
                preferred_element_type=jnp.float32,
            )
        )

    log_keep = decay_ref[0] * gate(rate_ref[0]) + extra_ref[...]
    state = jnp.sqrt(one_minus_exp(2.0 * log_keep)) * gate(inward_ref[0]) * convolved
    keep = jnp.exp(log_keep)
    lane = lax.broadcasted_iota(jnp.int32, keep.shape, 1)
    distance = 1
    while distance < positions:
        state = keep * shifted(state, 0.0, distance, lane) + state
        keep = keep * shifted(keep, 1.0, distance, lane)
        distance *= 2
    keep_ref[...] = keep
    state_ref[...] = state


def local_scan(edge, branch_input, conv_taps, rate_weight, input_weight, decay_rate, decay_extra):
    channels, positions = branch_input.shape
    blocks, width = rate_weight.shape[:2]
    taps = conv_taps.astype(jnp.float32).T.reshape(blocks, width, conv_taps.shape[0])
    pad = 128
    edge = jnp.pad(edge, ((0, 0), (pad - edge.shape[1], 0)))
    row = lambda i: (i, 0)
    block3 = lambda i: (i, 0, 0)
    return pl.pallas_call(
        scan_kernel,
        grid=(blocks,),
        in_specs=[
            pl.BlockSpec((width, pad), row),
            pl.BlockSpec((width, positions), row),
            pl.BlockSpec((1, width, taps.shape[2]), block3),
            pl.BlockSpec((1, width, width), block3),
            pl.BlockSpec((1, width, width), block3),
            pl.BlockSpec((1, width, 1), block3),
            pl.BlockSpec((1, positions), lambda i: (0, 0)),
        ],
        out_specs=[pl.BlockSpec((width, positions), row)] * 2,
        out_shape=[jax.ShapeDtypeStruct((channels, positions), jnp.float32)] * 2,
        cost_estimate=pl.CostEstimate(flops=channels * positions * 400, bytes_accessed=channels * positions * 12, transcendentals=channels * positions * 5),
    )(
        edge,
        branch_input,
        taps,
        rate_weight,
        input_weight,
        decay_rate.reshape(blocks, width, 1),
        decay_extra.reshape(1, positions),
    )


def expert_mlp(rows, gate_rows, up_rows, down_rows):
    contract = (((1,), (1,)), ((), ()))
    gate_vals = lax.dot_general(rows, gate_rows, contract, preferred_element_type=jnp.float32)
    up_vals = lax.dot_general(rows, up_rows, contract, preferred_element_type=jnp.float32)
    hidden = (jax.nn.silu(gate_vals) * up_vals).astype(jnp.bfloat16)
    return jnp.dot(hidden, down_rows, preferred_element_type=jnp.float32).astype(jnp.bfloat16)


def paired_moe(ffn_in, expert_ids, route_weight, gate_rows, up_rows, down_rows):
    tokens, width = ffn_in.shape
    devices = lax.axis_size("sp")
    groups = devices // 2
    cap = tokens // groups
    group = expert_ids[:, 0] // 2
    member = (group[:, None] == jnp.arange(groups, dtype=jnp.int32)[None, :]).astype(jnp.int32)
    slot = group * cap + jnp.sum((jnp.cumsum(member, axis=0) - 1) * member, axis=1)
    place = (slot[None, :] == jnp.arange(tokens, dtype=jnp.int32)[:, None]).astype(jnp.bfloat16)
    even = (expert_ids[:, 0] % 2 == 0)[:, None]
    by_expert = jnp.where(even, route_weight, route_weight[:, ::-1])
    extra = jnp.concatenate(split_three(by_expert), axis=1)
    extra = jnp.pad(extra, ((0, 0), (0, 128 - extra.shape[1])))
    outgoing = jnp.dot(place, jnp.concatenate([ffn_in, extra], axis=1), preferred_element_type=jnp.float32)
    outgoing = outgoing.astype(jnp.bfloat16)
    swap = [(i, i ^ 1) for i in range(devices)]
    mine = lax.all_to_all(outgoing, "sp", split_axis=0, concat_axis=0, tiled=True)
    rows = mine[:, :width]
    other_rows = lax.ppermute(rows, "sp", swap)
    other_out = expert_mlp(other_rows, gate_rows, up_rows, down_rows)
    from_other = lax.ppermute(other_out, "sp", swap)
    own_out = expert_mlp(rows, gate_rows, up_rows, down_rows)
    scale = mine[:, width : width + 6].astype(jnp.float32)
    scale = scale[:, 0:2] + scale[:, 2:4] + scale[:, 4:6]
    first = lax.axis_index("sp") % 2 == 0
    own_scale = jnp.where(first, scale[:, 0:1], scale[:, 1:2])
    other_scale = jnp.where(first, scale[:, 1:2], scale[:, 0:1])
    summed = own_scale * own_out.astype(jnp.float32) + other_scale * from_other.astype(jnp.float32)
    returned = lax.all_to_all(summed.astype(jnp.bfloat16), "sp", split_axis=0, concat_axis=0, tiled=True)
    return lax.dot_general(place, returned, (((0,), (0,)), ((), ())), preferred_element_type=jnp.float32)


def general_moe(ffn_in, expert_ids, route_weight, gate_rows, up_rows, down_rows):
    token_count = ffn_in.shape[0]
    top_count = expert_ids.shape[1]
    experts = gate_rows.shape[0] * lax.axis_size("sp")
    capacity = top_count * token_count // experts
    chosen = expert_ids.reshape(-1)
    matches = (chosen[:, None] == jnp.arange(experts, dtype=jnp.int32)[None, :]).astype(jnp.int32)
    slot_index = jnp.sum((jnp.cumsum(matches, axis=0) - 1) * matches, axis=1)
    target = chosen * capacity + slot_index
    source = (
        jnp.zeros((experts * capacity,), jnp.int32)
        .at[target]
        .set(jnp.arange(token_count * top_count, dtype=jnp.int32) // top_count)
    )
    outgoing = ffn_in[source].reshape(experts, capacity, ffn_in.shape[1])
    arriving = lax.all_to_all(outgoing, "sp", split_axis=0, concat_axis=1, tiled=True)
    gate_vals = jnp.einsum("emd,ekd->emk", arriving, gate_rows, preferred_element_type=jnp.float32)
    up_vals = jnp.einsum("emd,ekd->emk", arriving, up_rows, preferred_element_type=jnp.float32)
    hidden = (jax.nn.silu(gate_vals) * up_vals).astype(jnp.bfloat16)
    result = jnp.einsum("emk,ekd->emd", hidden, down_rows, preferred_element_type=jnp.float32)
    returned = lax.all_to_all(
        result.astype(jnp.bfloat16), "sp", split_axis=1, concat_axis=0, tiled=True
    )
    returned = returned.reshape(experts * capacity, returned.shape[2])
    picked = returned[target].astype(jnp.float32).reshape(token_count, top_count, returned.shape[1])
    return jnp.sum(picked * route_weight[:, :, None], axis=1)


expert_groups = 4


def per_device(
    resid,
    branch_input,
    gate_in,
    conv_taps,
    rate_weight,
    input_weight,
    decay_base,
    decay_extra,
    out_weight,
    gain_mix,
    gain_pre,
    gain_post,
    expert_ids,
    route_weight,
    gate_proj,
    up_proj,
    down_proj,
):
    channels, positions = branch_input.shape
    tap_count = conv_taps.shape[0]
    edge_cols = passed_along(branch_input[:, positions - (tap_count - 1) :], "sp", 1)
    decay_rate = -gate_power * jax.nn.softplus(-decay_base)
    keep, state = local_scan(
        edge_cols, branch_input, conv_taps, rate_weight, input_weight, decay_rate, decay_extra
    )
    _, entering = carry_in(keep[:, -1], state[:, -1])
    hidden_state = state + keep * entering[:, None]
    branch_out = (hidden_state * jax.nn.gelu(gate_in.astype(jnp.float32), approximate=True)).astype(
        jnp.bfloat16
    )
    token_rows = lax.all_to_all(branch_out, "tp", split_axis=1, concat_axis=0, tiled=True)
    token_count = token_rows.shape[1]
    mixed_rows = lax.dot_general(
        token_rows,
        lax.all_gather(out_weight, "tp", axis=0, tiled=True),
        (((0,), (0,)), ((), ())),
        preferred_element_type=jnp.float32,
    )
    after_mix = resid.astype(jnp.float32) + normalized(mixed_rows, gain_mix)
    ffn_in = normalized(after_mix, gain_pre).astype(jnp.bfloat16)
    gate_rows = lax.all_gather(gate_proj, "tp", axis=1, tiled=True)
    up_rows = lax.all_gather(up_proj, "tp", axis=1, tiled=True)
    down_rows = lax.all_gather(down_proj, "tp", axis=1, tiled=True)
    experts = gate_proj.shape[0] * lax.axis_size("sp")
    if gate_proj.shape[0] == 1 and experts // expert_groups == 2:
        moe = paired_moe(ffn_in, expert_ids, route_weight, gate_rows[0], up_rows[0], down_rows[0])
    else:
        moe = general_moe(ffn_in, expert_ids, route_weight, gate_rows, up_rows, down_rows)
    return (after_mix + normalized(moe, gain_post)).astype(jnp.bfloat16)


def layer_kernel(
    resid_ref, branch_ref, gatein_ref, taps_ref, rate_ref, inward_ref, decay_ref, extra_ref, outw_ref,
    gmix_ref, gpre_ref, gpost_ref, ids_ref, rw_ref, gate_ref, up_ref, down_ref, out_ref,
    edge, keep_s, state_s, carry, bo, br, owb, after_s, obuf, rows, gbuf, ubuf, dbuf, acc, res_send, res_recv, ret, back,
    edge_sem, carry_sem, br_sem, ow_sem, fwd_sem, w_sem, disp_sem, swap_sem, ret_sem,
):
    f32, bf16 = jnp.float32, jnp.bfloat16
    s, j = lax.axis_index("sp"), lax.axis_index("tp")
    sp = lax.axis_size("sp")
    c = s % 2
    partner = s + 1 - 2 * c
    jx, jy = j % 2, j // 2

    def tp_peer(k):
        x = 1 - jx if k % 2 else jx
        y = 1 - jy if k // 2 else jy
        return y * 2 + x

    def later(k):
        return (s + k) % sp

    def earlier(k):
        return (s + sp - k) % sp

    sent = []

    def send(src, dst, sem, at, device):
        copy = pltpu.make_async_remote_copy(
            src_ref=src, dst_ref=dst, send_sem=sem.at[0, at], recv_sem=sem.at[1, at],
            device_id=device, device_id_type=pl.DeviceIdType.MESH,
        )
        copy.start()
        sent.append(copy)
        return copy

    barrier = pltpu.get_barrier_semaphore()
    for k in range(1, 4):
        pl.semaphore_signal(barrier, inc=1, device_id=(s, tp_peer(k)), device_id_type=pl.DeviceIdType.MESH)
    for k in range(1, sp):
        pl.semaphore_signal(barrier, inc=1, device_id=(later(k), j), device_id_type=pl.DeviceIdType.MESH)
    pl.semaphore_wait(barrier, sp + 2)

    channels, positions = branch_ref.shape
    tile = 128
    edge_copy = send(branch_ref.at[:, positions - tile :], edge, edge_sem, 0, (later(1), j))
    half = channels // 2
    ow_in = {}
    for k in (3, 1, 2):
        ow_in[k] = send(outw_ref.at[pl.ds(c * half, half)], owb.at[k, c], ow_sem, k, (s, tp_peer(k)))
    w_in = {}
    for m, (ref, buf) in enumerate(((gate_ref, gbuf), (up_ref, ubuf), (down_ref, dbuf))):
        for k in (1, 2, 3):
            w_in[m, k] = send(ref.at[0], buf.at[k], w_sem, m * 4 + k, (s, tp_peer(k)))

    edge_copy.wait_recv()
    blocks, width = rate_ref.shape[0], rate_ref.shape[1]
    count = taps_ref.shape[2]
    started = jnp.where(s > 0, 1.0, 0.0)

    def scan_block(n, none):
        at = pl.ds(pl.multiple_of(n * width, width), width)
        taps = taps_ref[n]
        here = branch_ref[at, :].astype(f32)
        padded = jnp.concatenate([edge[at, :].astype(f32) * started, here], axis=1)
        convolved = taps[:, count - 1 : count] * here
        for step in range(1, count):
            moved = pltpu.roll(padded, step, 1)[:, tile:]
            convolved = convolved + taps[:, count - 1 - step : count - step] * moved
        stacked = jnp.concatenate(split_three(convolved), axis=0)

        def gate(weight):
            return jax.nn.sigmoid(
                lax.dot_general(
                    jnp.concatenate([weight] * 3, axis=0), stacked,
                    (((0,), (0,)), ((), ())), preferred_element_type=f32,
                )
            )

        log_keep = decay_ref[n] * gate(rate_ref[n]) + extra_ref[...]
        state = jnp.sqrt(one_minus_exp(2.0 * log_keep)) * gate(inward_ref[n]) * convolved
        keep = jnp.exp(log_keep)
        lane = lax.broadcasted_iota(jnp.int32, keep.shape, 1)
        distance = 1
        while distance < positions:
            state = keep * shifted(state, 0.0, distance, lane) + state
            keep = keep * shifted(keep, 1.0, distance, lane)
            distance *= 2
        keep_s[at, :] = keep
        state_s[at, :] = state
        return none

    lax.fori_loop(0, blocks, scan_block, 0)
    carry[0, 0:1, :] = keep_s[:, positions - tile :].T[tile - 1 : tile, :]
    carry[0, 1:2, :] = state_s[:, positions - tile :].T[tile - 1 : tile, :]
    carry_in_copies = {}
    for k in range(1, sp):
        carry_in_copies[k] = send(carry.at[0], carry.at[k], carry_sem, k, (later(k), j))
    entering = jnp.zeros((1, channels), f32)
    for k in range(sp - 1, 0, -1):
        carry_in_copies[k].wait_recv()
        entering = jnp.where(k <= s, carry[k, 0:1, :] * entering + carry[k, 1:2, :], entering)
    entering = jnp.broadcast_to(entering, (tile, channels)).T[:, 0:1]
    tokens = resid_ref.shape[0]
    for q in range(4):
        cols = slice(q * tokens, (q + 1) * tokens)
        hidden = state_s[:, cols] + keep_s[:, cols] * entering
        bo[q] = (hidden * jax.nn.gelu(gatein_ref[:, cols].astype(f32), approximate=True)).astype(bf16)
    br_in = {}
    for k in (3, 1, 2):
        br_in[k] = send(bo.at[tp_peer(k)], br.at[k], br_sem, k, (s, tp_peer(k)))
    br[0] = bo[j]
    owb[0, 0] = outw_ref[0:half, :]
    owb[0, 1] = outw_ref[half:, :]
    fwd = []
    for k in (3, 1, 2):
        ow_in[k].wait_recv()
        fwd.append(send(owb.at[k, c], owb.at[k, c], fwd_sem, k, (partner, j)))

    ids = ids_ref[...]
    first_id = ids[:, 0:1]
    group = first_id >> 1
    odd = first_id & 1
    lane = lax.broadcasted_iota(jnp.int32, (tokens, tokens), 1)
    sub = lax.broadcasted_iota(jnp.int32, (tokens, tokens), 0)
    member = jnp.where(lane == group, 1.0, 0.0)
    below = jnp.where(sub > lane, 1.0, 0.0).astype(bf16)
    prefix = jnp.dot(below, member.astype(bf16), preferred_element_type=f32)
    rank = jnp.sum(prefix * member, axis=1, keepdims=True)
    cap = tokens // (sp // 2)
    slot = group.astype(f32) * cap + rank
    place = jnp.where(slot == lane.astype(f32), 1.0, 0.0).astype(bf16)
    rw = rw_ref[...]
    w_even = jnp.where(odd == 0, rw[:, 0:1], rw[:, 1:2])
    w_odd = jnp.where(odd == 0, rw[:, 1:2], rw[:, 0:1])
    extra = jnp.zeros((tokens, tile), f32)
    lane_e = lax.broadcasted_iota(jnp.int32, (tokens, tile), 1)
    for at, piece in enumerate(split_three(w_even) + split_three(w_odd)):
        extra = jnp.where(lane_e == at, piece.astype(f32), extra)

    for k in (3, 1, 2):
        br_in[k].wait_recv()
    for copy in fwd:
        copy.wait_recv()
    features = resid_ref.shape[1]
    step = 512

    def mix_tile(t, none):
        cols = pl.ds(pl.multiple_of(t * step, step), step)
        total = jnp.zeros((tokens, step), f32)
        for k in range(4):
            for h in range(2):
                total = total + lax.dot_general(
                    br[k, h * half : (h + 1) * half, :], owb[k, h, :, cols],
                    (((0,), (0,)), ((), ())), preferred_element_type=f32,
                )
        after_s[:, cols] = total
        return none

    lax.fori_loop(0, features // step, mix_tile, 0)
    after_s[...] = resid_ref[...].astype(f32) + normalized(after_s[...], gmix_ref[...])
    acc_rows = normalized(after_s[...], gpre_ref[...]).astype(bf16)
    res_send[...] = acc_rows
    each = tokens // sp

    def place_rows(values):
        return lax.dot_general(place, values, (((0,), (0,)), ((), ())), preferred_element_type=f32).astype(bf16)

    def place_tile(t, none):
        cols = pl.ds(pl.multiple_of(t * step, step), step)
        obuf[:, :, cols] = place_rows(res_send[:, cols]).reshape(sp, each, step)
        return none

    lax.fori_loop(0, features // step, place_tile, 0)
    obuf[:, :, features:] = place_rows(extra.astype(bf16)).reshape(sp, each, tile)
    disp = []
    for k in range(sp - 1, 0, -1):
        disp.append(send(obuf.at[later(k)], rows.at[k], disp_sem, k, (later(k), j)))
    rows[0] = obuf[s]
    for copy in disp:
        copy.wait_recv()
    swap = send(rows.at[0:sp], rows.at[sp : 2 * sp], swap_sem, 0, (partner, j))
    swap.wait_recv()

    contract = (((1,), (1,)), ((), ()))
    for k in range(4):
        if k:
            w_in[0, k].wait_recv()
            w_in[1, k].wait_recv()
        gate_w = gbuf.at[k] if k else gate_ref.at[0]
        up_w = ubuf.at[k] if k else up_ref.at[0]
        down_w = dbuf.at[k] if k else down_ref.at[0]
        arrived = rows[:, :, 0:features].reshape(2 * tokens, features)
        gate_vals = lax.dot_general(arrived, gate_w[...], contract, preferred_element_type=f32)
        up_vals = lax.dot_general(arrived, up_w[...], contract, preferred_element_type=f32)
        hidden = (jax.nn.silu(gate_vals) * up_vals).astype(bf16)
        if k:
            w_in[2, k].wait_recv()

        def down_tile(t, none):
            cols = pl.ds(pl.multiple_of(t * step, step), step)
            part = jnp.dot(hidden, down_w[:, cols], preferred_element_type=f32)
            acc[:, cols] = part if k == 0 else acc[:, cols] + part
            return none

        lax.fori_loop(0, features // step, down_tile, 0)
    res_send[...] = acc[tokens:, :].astype(bf16)
    result = send(res_send, res_recv, swap_sem, 1, (partner, j))
    scales = rows[0:sp, :, features:].reshape(tokens, tile).astype(f32)
    s_even = jnp.sum(jnp.where(lane_e < 3, scales, 0.0), axis=1, keepdims=True)
    s_odd = jnp.sum(jnp.where((lane_e >= 3) & (lane_e < 6), scales, 0.0), axis=1, keepdims=True)
    own_scale = jnp.where(c == 0, s_even, s_odd)
    other_scale = jnp.where(c == 0, s_odd, s_even)
    own = own_scale * acc[0:tokens, :].astype(bf16).astype(f32)
    result.wait_recv()
    ret[...] = (own + other_scale * res_recv[...].astype(f32)).astype(bf16).reshape(sp, each, features)
    home = []
    for k in range(sp - 1, 0, -1):
        home.append(send(ret.at[k], back.at[s], ret_sem, k, (earlier(k), j)))
    back[s] = ret[0]
    for copy in home:
        copy.wait_recv()

    def gather_tile(t, none):
        cols = pl.ds(pl.multiple_of(t * step, step), step)
        acc[0:tokens, cols] = jnp.dot(place, back[:, :, cols].reshape(tokens, step), preferred_element_type=f32)
        return none

    lax.fori_loop(0, features // step, gather_tile, 0)
    out_ref[...] = (after_s[...] + normalized(acc[0:tokens, :], gpost_ref[...])).astype(out_ref.dtype)
    for copy in sent:
        copy.wait_send()


def fused_layer(
    resid, branch_input, gate_in, conv_taps, rate_weight, input_weight, decay_base, decay_extra, out_weight,
    gain_mix, gain_pre, gain_post, expert_ids, route_weight, gate_proj, up_proj, down_proj,
):
    channels, positions = branch_input.shape
    blocks, width = rate_weight.shape[:2]
    tokens, features = resid.shape
    sp = lax.axis_size("sp")
    hid = gate_proj.shape[1]
    each = tokens // sp
    f32, bf16 = jnp.float32, jnp.bfloat16
    taps = conv_taps.astype(f32).T.reshape(blocks, width, conv_taps.shape[0])
    decay_rate = (-gate_power * jax.nn.softplus(-decay_base)).reshape(blocks, width, 1)
    sems = lambda n: pltpu.SemaphoreType.DMA((2, n))
    vm = pltpu.VMEM
    return pl.pallas_call(
        layer_kernel,
        out_shape=jax.ShapeDtypeStruct((tokens, features), bf16),
        in_specs=[pl.BlockSpec(memory_space=pltpu.VMEM)] * 17,
        out_specs=pl.BlockSpec(memory_space=pltpu.VMEM),
        scratch_shapes=[
            vm((channels, 128), bf16),
            vm((channels, positions), f32),
            vm((channels, positions), f32),
            vm((sp, 8, channels), f32),
            vm((4, channels, tokens), bf16),
            vm((4, channels, tokens), bf16),
            vm((4, 2, channels // 2, features), bf16),
            vm((tokens, features), f32),
            vm((sp, each, features + 128), bf16),
            vm((2 * sp, each, features + 128), bf16),
            vm((4, hid, features), bf16),
            vm((4, hid, features), bf16),
            vm((4, hid, features), bf16),
            vm((2 * tokens, features), f32),
            vm((tokens, features), bf16),
            vm((tokens, features), bf16),
            vm((sp, each, features), bf16),
            vm((sp, each, features), bf16),
            sems(1), sems(sp), sems(4), sems(4), sems(4), sems(12), sems(sp), sems(2), sems(sp),
        ],
        compiler_params=pltpu.CompilerParams(
            collective_id=0, has_side_effects=True, vmem_limit_bytes=60 * 1024 * 1024
        ),
    )(
        resid, branch_input, gate_in, taps, rate_weight, input_weight, decay_rate,
        decay_extra.reshape(1, positions), out_weight, gain_mix.reshape(1, -1), gain_pre.reshape(1, -1),
        gain_post.reshape(1, -1), expert_ids, route_weight, gate_proj, up_proj, down_proj,
    )


def solution(mesh):
    in_specs = (
        P(("sp", "tp"), None),
        P("tp", "sp"),
        P("tp", "sp"),
        P(None, "tp"),
        P("tp", None, None),
        P("tp", None, None),
        P("tp"),
        P("sp"),
        P("tp", None),
        P(),
        P(),
        P(),
        P(("sp", "tp"), None),
        P(("sp", "tp"), None),
        P("sp", "tp", None),
        P("sp", "tp", None),
        P("sp", "tp", None),
    )
    out_specs = P(("sp", "tp"), None)
    paired = mesh.shape["tp"] == 4 and mesh.shape["sp"] == 2 * expert_groups
    return jax.shard_map(
        fused_layer if paired else per_device, mesh=mesh, in_specs=in_specs, out_specs=out_specs, check_vma=False
    )
```

```python
import jax
import jax.numpy as jnp
from jax import lax
from jax.experimental import pallas as pl
from jax.experimental.pallas import tpu as pltpu
from jax.sharding import PartitionSpec as P

epsilon = 1e-06
gate_power = 8.0


def entering_2(array, axis, combine, identity):
    count, here = (lax.axis_size(axis), lax.axis_index(axis))
    everything = jax.tree.map(lambda part: lax.all_gather(part, axis), array)
    start = jax.tree.map(
        lambda part, zero: jnp.broadcast_to(jnp.asarray(zero, part.dtype), part.shape),
        array,
        identity,
    )

    def hop(k, before):
        reached = k < here
        new = combine(before, jax.tree.map(lambda part: part[k], everything))
        return jax.tree.map(lambda a, b: jnp.where(reached, a, b), new, before)

    return lax.fori_loop(0, count, hop, start)


def passed_along(value, axis, steps):
    count = lax.axis_size(axis)
    first, last = (max(0, -steps), min(count, count - steps))
    return lax.ppermute(value, axis, [(source, source + steps) for source in range(first, last)])


def normalized(values, gain):
    return values * lax.rsqrt(jnp.mean(values * values, axis=-1, keepdims=True) + epsilon) * gain


def combine_pair(earlier, latter):
    return (earlier[0] * latter[0], latter[0] * earlier[1] + latter[1])


def carry_in(block_keep, block_state):
    identity = (jnp.ones(block_keep.shape, jnp.float32), jnp.zeros(block_state.shape, jnp.float32))
    return entering_2((block_keep, block_state), "sp", combine_pair, identity)


def shifted(values, fill, distance, lane):
    return jnp.where(lane >= distance, pltpu.roll(values, distance, 1), fill)


def one_minus_exp(y):
    small = 1.0 + y * (1.0 / 8.0)
    for k in range(7, 1, -1):
        small = 1.0 + y * (1.0 / k) * small
    return jnp.where(y > -0.5, -y * small, 1.0 - jnp.exp(y))


def split_three(values):
    high = values.astype(jnp.bfloat16)
    rest = values - high.astype(jnp.float32)
    mid = rest.astype(jnp.bfloat16)
    low = (rest - mid.astype(jnp.float32)).astype(jnp.bfloat16)
    return high, mid, low


def scan_kernel(edge_ref, input_ref, taps_ref, rate_ref, inward_ref, decay_ref, extra_ref, keep_ref, state_ref):
    taps = taps_ref[0]
    positions = input_ref.shape[1]
    here = input_ref[...].astype(jnp.float32)
    padded = jnp.concatenate([edge_ref[...].astype(jnp.float32), here], axis=1)
    pad = padded.shape[1] - positions
    count = taps.shape[1]
    convolved = taps[:, count - 1 : count] * here
    for back in range(1, count):
        moved = pltpu.roll(padded, back, 1)[:, pad:]
        convolved = convolved + taps[:, count - 1 - back : count - back] * moved
    stacked = jnp.concatenate(split_three(convolved), axis=0)

    def gate(weight):
        return jax.nn.sigmoid(
            lax.dot_general(
                jnp.concatenate([weight] * 3, axis=0),
                stacked,
                (((0,), (0,)), ((), ())),
                preferred_element_type=jnp.float32,
            )
        )

    log_keep = decay_ref[0] * gate(rate_ref[0]) + extra_ref[...]
    state = jnp.sqrt(one_minus_exp(2.0 * log_keep)) * gate(inward_ref[0]) * convolved
    keep = jnp.exp(log_keep)
    lane = lax.broadcasted_iota(jnp.int32, keep.shape, 1)
    distance = 1
    while distance < positions:
        state = keep * shifted(state, 0.0, distance, lane) + state
        keep = keep * shifted(keep, 1.0, distance, lane)
        distance *= 2
    keep_ref[...] = keep
    state_ref[...] = state


def local_scan(edge, branch_input, conv_taps, rate_weight, input_weight, decay_rate, decay_extra):
    channels, positions = branch_input.shape
    blocks, width = rate_weight.shape[:2]
    taps = conv_taps.astype(jnp.float32).T.reshape(blocks, width, conv_taps.shape[0])
    pad = 128
    edge = jnp.pad(edge, ((0, 0), (pad - edge.shape[1], 0)))
    row = lambda i: (i, 0)
    block3 = lambda i: (i, 0, 0)
    return pl.pallas_call(
        scan_kernel,
        grid=(blocks,),
        in_specs=[
            pl.BlockSpec((width, pad), row),
            pl.BlockSpec((width, positions), row),
            pl.BlockSpec((1, width, taps.shape[2]), block3),
            pl.BlockSpec((1, width, width), block3),
            pl.BlockSpec((1, width, width), block3),
            pl.BlockSpec((1, width, 1), block3),
            pl.BlockSpec((1, positions), lambda i: (0, 0)),
        ],
        out_specs=[pl.BlockSpec((width, positions), row)] * 2,
        out_shape=[jax.ShapeDtypeStruct((channels, positions), jnp.float32)] * 2,
        cost_estimate=pl.CostEstimate(flops=channels * positions * 400, bytes_accessed=channels * positions * 12, transcendentals=channels * positions * 5),
    )(
        edge,
        branch_input,
        taps,
        rate_weight,
        input_weight,
        decay_rate.reshape(blocks, width, 1),
        decay_extra.reshape(1, positions),
    )


def expert_mlp(rows, gate_rows, up_rows, down_rows):
    contract = (((1,), (1,)), ((), ()))
    gate_vals = lax.dot_general(rows, gate_rows, contract, preferred_element_type=jnp.float32)
    up_vals = lax.dot_general(rows, up_rows, contract, preferred_element_type=jnp.float32)
    hidden = (jax.nn.silu(gate_vals) * up_vals).astype(jnp.bfloat16)
    return jnp.dot(hidden, down_rows, preferred_element_type=jnp.float32).astype(jnp.bfloat16)


def paired_moe(ffn_in, expert_ids, route_weight, gate_rows, up_rows, down_rows):
    tokens, width = ffn_in.shape
    devices = lax.axis_size("sp")
    groups = devices // 2
    cap = tokens // groups
    group = expert_ids[:, 0] // 2
    member = (group[:, None] == jnp.arange(groups, dtype=jnp.int32)[None, :]).astype(jnp.int32)
    slot = group * cap + jnp.sum((jnp.cumsum(member, axis=0) - 1) * member, axis=1)
    place = (slot[None, :] == jnp.arange(tokens, dtype=jnp.int32)[:, None]).astype(jnp.bfloat16)
    even = (expert_ids[:, 0] % 2 == 0)[:, None]
    by_expert = jnp.where(even, route_weight, route_weight[:, ::-1])
    extra = jnp.concatenate(split_three(by_expert), axis=1)
    extra = jnp.pad(extra, ((0, 0), (0, 128 - extra.shape[1])))
    outgoing = jnp.dot(place, jnp.concatenate([ffn_in, extra], axis=1), preferred_element_type=jnp.float32)
    outgoing = outgoing.astype(jnp.bfloat16)
    swap = [(i, i ^ 1) for i in range(devices)]
    mine = lax.all_to_all(outgoing, "sp", split_axis=0, concat_axis=0, tiled=True)
    rows = mine[:, :width]
    other_rows = lax.ppermute(rows, "sp", swap)
    other_out = expert_mlp(other_rows, gate_rows, up_rows, down_rows)
    from_other = lax.ppermute(other_out, "sp", swap)
    own_out = expert_mlp(rows, gate_rows, up_rows, down_rows)
    scale = mine[:, width : width + 6].astype(jnp.float32)
    scale = scale[:, 0:2] + scale[:, 2:4] + scale[:, 4:6]
    first = lax.axis_index("sp") % 2 == 0
    own_scale = jnp.where(first, scale[:, 0:1], scale[:, 1:2])
    other_scale = jnp.where(first, scale[:, 1:2], scale[:, 0:1])
    summed = own_scale * own_out.astype(jnp.float32) + other_scale * from_other.astype(jnp.float32)
    returned = lax.all_to_all(summed.astype(jnp.bfloat16), "sp", split_axis=0, concat_axis=0, tiled=True)
    return lax.dot_general(place, returned, (((0,), (0,)), ((), ())), preferred_element_type=jnp.float32)


def general_moe(ffn_in, expert_ids, route_weight, gate_rows, up_rows, down_rows):
    token_count = ffn_in.shape[0]
    top_count = expert_ids.shape[1]
    experts = gate_rows.shape[0] * lax.axis_size("sp")
    capacity = top_count * token_count // experts
    chosen = expert_ids.reshape(-1)
    matches = (chosen[:, None] == jnp.arange(experts, dtype=jnp.int32)[None, :]).astype(jnp.int32)
    slot_index = jnp.sum((jnp.cumsum(matches, axis=0) - 1) * matches, axis=1)
    target = chosen * capacity + slot_index
    source = (
        jnp.zeros((experts * capacity,), jnp.int32)
        .at[target]
        .set(jnp.arange(token_count * top_count, dtype=jnp.int32) // top_count)
    )
    outgoing = ffn_in[source].reshape(experts, capacity, ffn_in.shape[1])
    arriving = lax.all_to_all(outgoing, "sp", split_axis=0, concat_axis=1, tiled=True)
    gate_vals = jnp.einsum("emd,ekd->emk", arriving, gate_rows, preferred_element_type=jnp.float32)
    up_vals = jnp.einsum("emd,ekd->emk", arriving, up_rows, preferred_element_type=jnp.float32)
    hidden = (jax.nn.silu(gate_vals) * up_vals).astype(jnp.bfloat16)
    result = jnp.einsum("emk,ekd->emd", hidden, down_rows, preferred_element_type=jnp.float32)
    returned = lax.all_to_all(
        result.astype(jnp.bfloat16), "sp", split_axis=1, concat_axis=0, tiled=True
    )
    returned = returned.reshape(experts * capacity, returned.shape[2])
    picked = returned[target].astype(jnp.float32).reshape(token_count, top_count, returned.shape[1])
    return jnp.sum(picked * route_weight[:, :, None], axis=1)


expert_groups = 4


def per_device(
    resid,
    branch_input,
    gate_in,
    conv_taps,
    rate_weight,
    input_weight,
    decay_base,
    decay_extra,
    out_weight,
    gain_mix,
    gain_pre,
    gain_post,
    expert_ids,
    route_weight,
    gate_proj,
    up_proj,
    down_proj,
):
    channels, positions = branch_input.shape
    tap_count = conv_taps.shape[0]
    edge_cols = passed_along(branch_input[:, positions - (tap_count - 1) :], "sp", 1)
    decay_rate = -gate_power * jax.nn.softplus(-decay_base)
    keep, state = local_scan(
        edge_cols, branch_input, conv_taps, rate_weight, input_weight, decay_rate, decay_extra
    )
    _, entering = carry_in(keep[:, -1], state[:, -1])
    hidden_state = state + keep * entering[:, None]
    branch_out = (hidden_state * jax.nn.gelu(gate_in.astype(jnp.float32), approximate=True)).astype(
        jnp.bfloat16
    )
    token_rows = lax.all_to_all(branch_out, "tp", split_axis=1, concat_axis=0, tiled=True)
    token_count = token_rows.shape[1]
    mixed_rows = lax.dot_general(
        token_rows,
        lax.all_gather(out_weight, "tp", axis=0, tiled=True),
        (((0,), (0,)), ((), ())),
        preferred_element_type=jnp.float32,
    )
    after_mix = resid.astype(jnp.float32) + normalized(mixed_rows, gain_mix)
    ffn_in = normalized(after_mix, gain_pre).astype(jnp.bfloat16)
    gate_rows = lax.all_gather(gate_proj, "tp", axis=1, tiled=True)
    up_rows = lax.all_gather(up_proj, "tp", axis=1, tiled=True)
    down_rows = lax.all_gather(down_proj, "tp", axis=1, tiled=True)
    experts = gate_proj.shape[0] * lax.axis_size("sp")
    if gate_proj.shape[0] == 1 and experts // expert_groups == 2:
        moe = paired_moe(ffn_in, expert_ids, route_weight, gate_rows[0], up_rows[0], down_rows[0])
    else:
        moe = general_moe(ffn_in, expert_ids, route_weight, gate_rows, up_rows, down_rows)
    return (after_mix + normalized(moe, gain_post)).astype(jnp.bfloat16)


def layer_kernel(
    resid_ref, branch_ref, gatein_ref, taps_ref, rate_ref, inward_ref, decay_ref, extra_ref, outw_ref,
    gmix_ref, gpre_ref, gpost_ref, ids_ref, rw_ref, gate_ref, up_ref, down_ref, out_ref,
    edge, keep_s, state_s, carry, bo, br, owb, after_s, obuf, rows, gbuf, ubuf, dbuf, acc, res_send, res_recv, ret, back,
    edge_sem, carry_sem, br_sem, ow_sem, fwd_sem, w_sem, disp_sem, swap_sem, ret_sem,
):
    f32, bf16 = jnp.float32, jnp.bfloat16
    s, j = lax.axis_index("sp"), lax.axis_index("tp")
    sp = lax.axis_size("sp")
    c = s % 2
    partner = s + 1 - 2 * c
    jx, jy = j % 2, j // 2

    def tp_peer(k):
        x = 1 - jx if k % 2 else jx
        y = 1 - jy if k // 2 else jy
        return y * 2 + x

    def later(k):
        return (s + k) % sp

    def earlier(k):
        return (s + sp - k) % sp

    sent = []

    def send(src, dst, sem, at, device):
        copy = pltpu.make_async_remote_copy(
            src_ref=src, dst_ref=dst, send_sem=sem.at[0, at], recv_sem=sem.at[1, at],
            device_id=device, device_id_type=pl.DeviceIdType.MESH,
        )
        copy.start()
        sent.append(copy)
        return copy

    barrier = pltpu.get_barrier_semaphore()
    for k in range(1, 4):
        pl.semaphore_signal(barrier, inc=1, device_id=(s, tp_peer(k)), device_id_type=pl.DeviceIdType.MESH)
    for k in range(1, sp):
        pl.semaphore_signal(barrier, inc=1, device_id=(later(k), j), device_id_type=pl.DeviceIdType.MESH)
    pl.semaphore_wait(barrier, sp + 2)

    channels, positions = branch_ref.shape
    tile = 128
    edge_copy = send(branch_ref.at[:, positions - tile :], edge, edge_sem, 0, (later(1), j))
    half = channels // 2
    ow_in = {}
    for k in (3, 1, 2):
        ow_in[k] = send(outw_ref.at[pl.ds(c * half, half)], owb.at[k, c], ow_sem, k, (s, tp_peer(k)))
    w_in = {}
    weights = ((gate_ref, gbuf), (up_ref, ubuf), (down_ref, dbuf))
    hid_half = gate_ref.shape[1] // 2

    def send_weight(m):
        ref, buf = weights[m]
        for k in (1, 2):
            w_in[m, k] = send(ref.at[0], buf.at[k], w_sem, m * 4 + k, (s, tp_peer(k)))

    def relay_weight(m):
        buf = weights[m][1]
        upper, lower = pl.ds(0, hid_half), pl.ds(hid_half, hid_half)
        w_in[m, 1].wait_recv()
        w_in[m, 3] = send(buf.at[1, upper], buf.at[3, upper], w_sem, m * 4 + 3, (s, tp_peer(2)))
        w_in[m, 2].wait_recv()
        w_in[m, 0] = send(buf.at[2, lower], buf.at[3, lower], w_sem, m * 4, (s, tp_peer(1)))

    edge_copy.wait_recv()
    blocks, width = rate_ref.shape[0], rate_ref.shape[1]
    count = taps_ref.shape[2]
    started = jnp.where(s > 0, 1.0, 0.0)

    def scan_block(n, none):
        at = pl.ds(pl.multiple_of(n * width, width), width)
        taps = taps_ref[n]
        here = branch_ref[at, :].astype(f32)
        padded = jnp.concatenate([edge[at, :].astype(f32) * started, here], axis=1)
        convolved = taps[:, count - 1 : count] * here
        for step in range(1, count):
            moved = pltpu.roll(padded, step, 1)[:, tile:]
            convolved = convolved + taps[:, count - 1 - step : count - step] * moved
        stacked = jnp.concatenate(split_three(convolved), axis=0)

        def gate(weight):
            return jax.nn.sigmoid(
                lax.dot_general(
                    jnp.concatenate([weight] * 3, axis=0), stacked,
                    (((0,), (0,)), ((), ())), preferred_element_type=f32,
                )
            )

        log_keep = decay_ref[n] * gate(rate_ref[n]) + extra_ref[...]
        state = jnp.sqrt(one_minus_exp(2.0 * log_keep)) * gate(inward_ref[n]) * convolved
        keep = jnp.exp(log_keep)
        lane = lax.broadcasted_iota(jnp.int32, keep.shape, 1)
        distance = 1
        while distance < positions:
            state = keep * shifted(state, 0.0, distance, lane) + state
            keep = keep * shifted(keep, 1.0, distance, lane)
            distance *= 2
        keep_s[at, :] = keep
        state_s[at, :] = state
        return none

    lax.fori_loop(0, blocks, scan_block, 0)
    carry[0, 0:1, :] = keep_s[:, positions - tile :].T[tile - 1 : tile, :]
    carry[0, 1:2, :] = state_s[:, positions - tile :].T[tile - 1 : tile, :]
    carry_in_copies = {}
    for k in range(1, sp):
        carry_in_copies[k] = send(carry.at[0], carry.at[k], carry_sem, k, (later(k), j))
    entering = jnp.zeros((1, channels), f32)
    for k in range(sp - 1, 0, -1):
        carry_in_copies[k].wait_recv()
        entering = jnp.where(k <= s, carry[k, 0:1, :] * entering + carry[k, 1:2, :], entering)
    entering = jnp.broadcast_to(entering, (tile, channels)).T[:, 0:1]
    tokens = resid_ref.shape[0]
    for q in range(4):
        cols = slice(q * tokens, (q + 1) * tokens)
        hidden = state_s[:, cols] + keep_s[:, cols] * entering
        bo[q] = (hidden * jax.nn.gelu(gatein_ref[:, cols].astype(f32), approximate=True)).astype(bf16)
    br_in = {}
    for k in (3, 1, 2):
        br_in[k] = send(bo.at[tp_peer(k)], br.at[k], br_sem, k, (s, tp_peer(k)))
    send_weight(0)
    send_weight(1)
    br[0] = bo[j]
    owb[0, 0] = outw_ref[0:half, :]
    owb[0, 1] = outw_ref[half:, :]
    fwd = []
    for k in (3, 1, 2):
        ow_in[k].wait_recv()
        fwd.append(send(owb.at[k, c], owb.at[k, c], fwd_sem, k, (partner, j)))

    ids = ids_ref[...]
    first_id = ids[:, 0:1]
    group = first_id >> 1
    odd = first_id & 1
    lane = lax.broadcasted_iota(jnp.int32, (tokens, tokens), 1)
    sub = lax.broadcasted_iota(jnp.int32, (tokens, tokens), 0)
    member = jnp.where(lane == group, 1.0, 0.0)
    below = jnp.where(sub > lane, 1.0, 0.0).astype(bf16)
    prefix = jnp.dot(below, member.astype(bf16), preferred_element_type=f32)
    rank = jnp.sum(prefix * member, axis=1, keepdims=True)
    cap = tokens // (sp // 2)
    slot = group.astype(f32) * cap + rank
    place = jnp.where(slot == lane.astype(f32), 1.0, 0.0).astype(bf16)
    rw = rw_ref[...]
    w_even = jnp.where(odd == 0, rw[:, 0:1], rw[:, 1:2])
    w_odd = jnp.where(odd == 0, rw[:, 1:2], rw[:, 0:1])
    extra = jnp.zeros((tokens, tile), f32)
    lane_e = lax.broadcasted_iota(jnp.int32, (tokens, tile), 1)
    for at, piece in enumerate(split_three(w_even) + split_three(w_odd)):
        extra = jnp.where(lane_e == at, piece.astype(f32), extra)

    for k in (3, 1, 2):
        br_in[k].wait_recv()
    for copy in fwd:
        copy.wait_recv()
    features = resid_ref.shape[1]
    step = 512

    def mix_tile(t, none):
        cols = pl.ds(pl.multiple_of(t * step, step), step)
        total = jnp.zeros((tokens, step), f32)
        for k in range(4):
            for h in range(2):
                total = total + lax.dot_general(
                    br[k, h * half : (h + 1) * half, :], owb[k, h, :, cols],
                    (((0,), (0,)), ((), ())), preferred_element_type=f32,
                )
        after_s[:, cols] = total
        return none

    lax.fori_loop(0, features // step, mix_tile, 0)
    after_s[...] = resid_ref[...].astype(f32) + normalized(after_s[...], gmix_ref[...])
    acc_rows = normalized(after_s[...], gpre_ref[...]).astype(bf16)
    res_send[...] = acc_rows
    each = tokens // sp

    def place_rows(values):
        return lax.dot_general(place, values, (((0,), (0,)), ((), ())), preferred_element_type=f32).astype(bf16)

    def place_tile(t, none):
        cols = pl.ds(pl.multiple_of(t * step, step), step)
        obuf[:, :, cols] = place_rows(res_send[:, cols]).reshape(sp, each, step)
        return none

    lax.fori_loop(0, features // step, place_tile, 0)
    obuf[:, :, features:] = place_rows(extra.astype(bf16)).reshape(sp, each, tile)
    disp = []
    for k in range(sp - 1, 0, -1):
        disp.append(send(obuf.at[later(k)], rows.at[k], disp_sem, k, (later(k), j)))
    rows[0] = obuf[s]
    relay_weight(0)
    relay_weight(1)
    send_weight(2)
    for copy in disp:
        copy.wait_recv()
    swap = send(rows.at[0:sp], rows.at[sp : 2 * sp], swap_sem, 0, (partner, j))
    swap.wait_recv()

    contract = (((1,), (1,)), ((), ()))
    hiddens = []
    for k in range(4):
        if k == 3:
            for at in (3, 0):
                w_in[0, at].wait_recv()
                w_in[1, at].wait_recv()
        gate_w = gbuf.at[k] if k else gate_ref.at[0]
        up_w = ubuf.at[k] if k else up_ref.at[0]
        arrived = rows[:, :, 0:features].reshape(2 * tokens, features)
        gate_vals = lax.dot_general(arrived, gate_w[...], contract, preferred_element_type=f32)
        up_vals = lax.dot_general(arrived, up_w[...], contract, preferred_element_type=f32)
        hiddens.append((jax.nn.silu(gate_vals) * up_vals).astype(bf16))
    for k in range(4):
        if k == 1:
            relay_weight(2)
        if k == 3:
            w_in[2, 3].wait_recv()
            w_in[2, 0].wait_recv()
        down_w = dbuf.at[k] if k else down_ref.at[0]

        def down_tile(t, none):
            cols = pl.ds(pl.multiple_of(t * step, step), step)
            part = jnp.dot(hiddens[k], down_w[:, cols], preferred_element_type=f32)
            acc[:, cols] = part if k == 0 else acc[:, cols] + part
            return none

        lax.fori_loop(0, features // step, down_tile, 0)
    res_send[...] = acc[tokens:, :].astype(bf16)
    result = send(res_send, res_recv, swap_sem, 1, (partner, j))
    scales = rows[0:sp, :, features:].reshape(tokens, tile).astype(f32)
    s_even = jnp.sum(jnp.where(lane_e < 3, scales, 0.0), axis=1, keepdims=True)
    s_odd = jnp.sum(jnp.where((lane_e >= 3) & (lane_e < 6), scales, 0.0), axis=1, keepdims=True)
    own_scale = jnp.where(c == 0, s_even, s_odd)
    other_scale = jnp.where(c == 0, s_odd, s_even)
    own = own_scale * acc[0:tokens, :].astype(bf16).astype(f32)
    result.wait_recv()
    ret[...] = (own + other_scale * res_recv[...].astype(f32)).astype(bf16).reshape(sp, each, features)
    home = []
    for k in range(sp - 1, 0, -1):
        home.append(send(ret.at[k], back.at[s], ret_sem, k, (earlier(k), j)))
    back[s] = ret[0]
    for copy in home:
        copy.wait_recv()

    def gather_tile(t, none):
        cols = pl.ds(pl.multiple_of(t * step, step), step)
        acc[0:tokens, cols] = jnp.dot(place, back[:, :, cols].reshape(tokens, step), preferred_element_type=f32)
        return none

    lax.fori_loop(0, features // step, gather_tile, 0)
    out_ref[...] = (after_s[...] + normalized(acc[0:tokens, :], gpost_ref[...])).astype(out_ref.dtype)
    for copy in sent:
        copy.wait_send()


def fused_layer(
    resid, branch_input, gate_in, conv_taps, rate_weight, input_weight, decay_base, decay_extra, out_weight,
    gain_mix, gain_pre, gain_post, expert_ids, route_weight, gate_proj, up_proj, down_proj,
):
    channels, positions = branch_input.shape
    blocks, width = rate_weight.shape[:2]
    tokens, features = resid.shape
    sp = lax.axis_size("sp")
    hid = gate_proj.shape[1]
    each = tokens // sp
    f32, bf16 = jnp.float32, jnp.bfloat16
    taps = conv_taps.astype(f32).T.reshape(blocks, width, conv_taps.shape[0])
    decay_rate = (-gate_power * jax.nn.softplus(-decay_base)).reshape(blocks, width, 1)
    sems = lambda n: pltpu.SemaphoreType.DMA((2, n))
    vm = pltpu.VMEM
    return pl.pallas_call(
        layer_kernel,
        out_shape=jax.ShapeDtypeStruct((tokens, features), bf16),
        in_specs=[pl.BlockSpec(memory_space=pltpu.VMEM)] * 17,
        out_specs=pl.BlockSpec(memory_space=pltpu.VMEM),
        scratch_shapes=[
            vm((channels, 128), bf16),
            vm((channels, positions), f32),
            vm((channels, positions), f32),
            vm((sp, 8, channels), f32),
            vm((4, channels, tokens), bf16),
            vm((4, channels, tokens), bf16),
            vm((4, 2, channels // 2, features), bf16),
            vm((tokens, features), f32),
            vm((sp, each, features + 128), bf16),
            vm((2 * sp, each, features + 128), bf16),
            vm((4, hid, features), bf16),
            vm((4, hid, features), bf16),
            vm((4, hid, features), bf16),
            vm((2 * tokens, features), f32),
            vm((tokens, features), bf16),
            vm((tokens, features), bf16),
            vm((sp, each, features), bf16),
            vm((sp, each, features), bf16),
            sems(1), sems(sp), sems(4), sems(4), sems(4), sems(12), sems(sp), sems(2), sems(sp),
        ],
        compiler_params=pltpu.CompilerParams(
            collective_id=0, has_side_effects=True, vmem_limit_bytes=60 * 1024 * 1024
        ),
    )(
        resid, branch_input, gate_in, taps, rate_weight, input_weight, decay_rate,
        decay_extra.reshape(1, positions), out_weight, gain_mix.reshape(1, -1), gain_pre.reshape(1, -1),
        gain_post.reshape(1, -1), expert_ids, route_weight, gate_proj, up_proj, down_proj,
    )


def solution(mesh):
    in_specs = (
        P(("sp", "tp"), None),
        P("tp", "sp"),
        P("tp", "sp"),
        P(None, "tp"),
        P("tp", None, None),
        P("tp", None, None),
        P("tp"),
        P("sp"),
        P("tp", None),
        P(),
        P(),
        P(),
        P(("sp", "tp"), None),
        P(("sp", "tp"), None),
        P("sp", "tp", None),
        P("sp", "tp", None),
        P("sp", "tp", None),
    )
    out_specs = P(("sp", "tp"), None)
    paired = mesh.shape["tp"] == 4 and mesh.shape["sp"] == 2 * expert_groups
    return jax.shard_map(
        fused_layer if paired else per_device, mesh=mesh, in_specs=in_specs, out_specs=out_specs, check_vma=False
    )
```
